1024 devices in a mesh: ep: 32 (over z, core), tp: 32 (over y, x).
Axes of the slice: x: 4, y: 8, z: 16, core: 2. Of those that a mesh axis runs over, the one named last changes fastest.
Arguments:
- stream: bfloat16 [512, 4096], P('ep'), may hold values from -6 to 6
- previous_state: float32 [512, 128, 4096], P('ep', None, 'tp'), may hold values from -6 to 6
- mixer_norm_gain: float32 [4096], replicated, may hold values from 0.1 to 1.9
- query_matrix: bfloat16 [4096, 2048], P('ep'), may hold values from -0.09375 to 0.09375
- key_matrix: bfloat16 [4096, 2048], P('ep'), may hold values from -0.09375 to 0.09375
- value_matrix: bfloat16 [4096, 4096], P('ep', 'tp'), may hold values from -0.09375 to 0.09375
- output_gate_weight: bfloat16 [4096, 4096], P('ep', 'tp'), may hold values from -0.09375 to 0.09375
- decay_lower_factor: bfloat16 [4096, 64], replicated, may hold values from -0.09375 to 0.09375
- decay_upper_factor: bfloat16 [64, 2048], replicated, may hold values from -3 to 3
- forgetting_boost: float32 [512, 2048], P('ep'), may hold values from 0.02 to 1.5
- head_norm_gain: float32 [256], replicated, may hold values from 0.1 to 1.9
- output_matrix: bfloat16 [4096, 4096], P('tp'), may hold values from -0.1875 to 0.1875
- mixture_norm_gain: float32 [4096], replicated, may hold values from 0.1 to 1.9
- expert_gate_weight: bfloat16 [32, 1024, 4096], P('ep', 'tp'), may hold values from -0.09375 to 0.09375
- expert_up_weight: bfloat16 [32, 1024, 4096], P('ep', 'tp'), may hold values from -0.09375 to 0.09375
- expert_down_weight: bfloat16 [32, 1024, 4096], P('ep', None, 'tp'), may hold values from -0.375 to 0.375
- expert_index_table: int32 [512, 2], P('ep'), may hold values from 0 to 31, as said below
- expert_scores_within: float32 [512, 2], P('ep'), may hold values from -6 to 6
- group_probability: float32 [512], P('ep'), may hold values from 0.3 to 1
Outputs:
- new_stream: bfloat16 [512, 4096], P('ep', 'tp')
- new_state: float32 [512, 128, 4096], P('ep', None, 'tp')
The draws below stay inside these ranges and needn't reach their ends.
Inputs may be any that keep to these rules, and one draw needn't show every extreme that they name: `expert_index_table`: the 2 experts of a sequence are distinct and lie in one group of 8 consecutive experts. Among the 16 sequences of one index of ep (aligned blocks of rows), each expert is named at most 2 times, and in every block some experts are named exactly 2 times.
All inputs are finite; a program needn't handle non-finite values.
Results may differ from the reference program's by a relative error of at most 0.02.
Values may be sent and summed in bfloat16 or wider, within the bound.
A program may use at most 32 MiB of HBM per device.

```python
import math
import jax
import jax.numpy as jnp
from jax import lax

D = 4096
HEAD_TOTAL = 16
KEY_CHANNELS = 128
DV = 256
RANK = 64
FF = 1024
GROUPS = 4
TOPK = 2
SEQ_DEV = 16
SEQUENCE_TOTAL = 512
EXPERTS = 32
PER_GROUP = 8
CAP = 2
N_EP = 32


def shuffle(subkey):
    return jax.random.permutation(subkey, SEQ_DEV)


def draw_expert_index_table(key, part):
    blocks = SEQUENCE_TOTAL // SEQ_DEV
    hot_count = PER_GROUP * CAP // TOPK
    key_hot, key_other, key_perm, key_turn = jax.random.split(jax.random.fold_in(key, 11), 4)
    hot_group = jax.random.randint(key_hot, (), 0, GROUPS)
    offsets = jax.random.randint(key_other, (blocks, SEQ_DEV), 1, GROUPS)
    orders = jax.vmap(shuffle)(jax.random.split(key_perm, blocks))
    places = jnp.arange(SEQ_DEV)
    chosen = (orders[:, :, None] == places[None, None, :]) & (places[None, :, None] < hot_count)
    is_hot = jnp.any(chosen, axis=1)
    group_id = jnp.where(is_hot, hot_group, (hot_group + offsets) % GROUPS)
    same_group = group_id[:, :, None] == group_id[:, None, :]
    before = places[None, :] < places[:, None]
    rank_in = jnp.sum(same_group & before[None], axis=2)
    rotation = jax.random.randint(key_turn, (blocks, GROUPS), 0, PER_GROUP)
    member = group_id[:, :, None] == jnp.arange(GROUPS)[None, None, :]
    shift_by = jnp.sum(jnp.where(member, rotation[:, None, :], 0), axis=2)
    within = (shift_by[:, :, None] + rank_in[:, :, None] * TOPK + jnp.arange(TOPK)[None, None, :]) % PER_GROUP
    chosen_ids = group_id[:, :, None] * PER_GROUP + within
    return chosen_ids.reshape(SEQUENCE_TOTAL, TOPK).astype(jnp.int32)


def block_scale(rng, dims, pieces, least, high):
    def one(position, shards_of):
        steps = jax.random.uniform(jax.random.fold_in(jax.random.fold_in(rng, 6), position), (shards_of,), jnp.float32, least / len(pieces), high / len(pieces))
        return jnp.repeat(jnp.exp(steps), dims[position] // shards_of).reshape((-1,) + (1,) * (len(dims) - position - 1))

    level = one(*pieces[0])
    for cut in pieces[1:]:
        level = level * one(*cut)
    return level


def centred(stream_key, dims, width, limit, cuts=(), kind=jnp.bfloat16):
    result = jax.random.normal(stream_key, dims, jnp.float32) * width
    if len(cuts) > 0:
        result = block_scale(stream_key, dims, cuts, -0.22, 0.18) * result
    return jnp.clip(result, min=-limit, max=limit).astype(kind)


def setup_inputs(seed: int = 0) -> dict:
    key_list = jax.random.split(jax.random.key(seed), 20)
    return {
        "stream": centred(key_list[0], (SEQUENCE_TOTAL, D), 1.0, 6.0, ((0, 32),)),
        "previous_state": centred(key_list[1], (SEQUENCE_TOTAL, KEY_CHANNELS, HEAD_TOTAL * DV), 1.0, 6.0, ((0, 32), (2, 32)), jnp.float32),
        "mixer_norm_gain": jnp.clip(1.0 + 0.18 * jax.random.normal(key_list[2], (D,), jnp.float32), 0.1, 1.9),
        "query_matrix": centred(key_list[3], (D, HEAD_TOTAL * KEY_CHANNELS), D ** -0.5, 0.09375, ((0, 32),)),
        "key_matrix": centred(key_list[4], (D, HEAD_TOTAL * KEY_CHANNELS), D ** -0.5, 0.09375, ((0, 32),)),
        "value_matrix": centred(key_list[5], (D, HEAD_TOTAL * DV), D ** -0.5, 0.09375, ((0, 32), (1, 32))),
        "output_gate_weight": centred(key_list[6], (D, HEAD_TOTAL * DV), D ** -0.5, 0.09375, ((0, 32), (1, 32))),
        "decay_lower_factor": centred(key_list[7], (D, RANK), D ** -0.5, 0.09375),
        "decay_upper_factor": centred(key_list[8], (RANK, HEAD_TOTAL * KEY_CHANNELS), (RANK // 16) ** -0.5, 3.0),
        "forgetting_boost": jnp.clip(jnp.exp(math.log(1.5) - 4.317488 * jax.random.uniform(key_list[9], (SEQUENCE_TOTAL, HEAD_TOTAL * KEY_CHANNELS), jnp.float32) ** block_scale(key_list[9], (SEQUENCE_TOTAL, HEAD_TOTAL * KEY_CHANNELS), ((0, 32),), -0.2, 0.2)), 0.02, 1.5),
        "head_norm_gain": jnp.clip(1.0 + 0.18 * jax.random.normal(key_list[10], (DV,), jnp.float32), 0.1, 1.9),
        "output_matrix": centred(key_list[11], (HEAD_TOTAL * DV, D), (HEAD_TOTAL * DV // 4) ** -0.5, 0.1875, ((0, 32),)),
        "mixture_norm_gain": jnp.clip(1.0 + 0.18 * jax.random.normal(key_list[12], (D,), jnp.float32), 0.1, 1.9),
        "expert_gate_weight": centred(key_list[13], (EXPERTS, FF, D), D ** -0.5, 0.09375, ((0, 32), (1, 32))),
        "expert_up_weight": centred(key_list[14], (EXPERTS, FF, D), D ** -0.5, 0.09375, ((0, 32), (1, 32))),
        "expert_down_weight": centred(key_list[15], (EXPERTS, FF, D), (FF // 4) ** -0.5, 0.375, ((0, 32), (2, 32))),
        "expert_index_table": draw_expert_index_table(jax.random.fold_in(key_list[19], 71), 0),
        "expert_scores_within": centred(key_list[17], (SEQUENCE_TOTAL, TOPK), 1.5, 6.0, ((0, 32),), jnp.float32),
        "group_probability": jnp.clip(0.3 + 0.7 * jax.random.uniform(key_list[18], (SEQUENCE_TOTAL,), jnp.float32) ** block_scale(key_list[18], (SEQUENCE_TOTAL,), ((0, 32),), -0.2, 0.2), 0.3, 1.0),
    }


epsilon = 1e-06
forgetting_softness = 16.0

def rms_scaled(values, gain_vec):
    floats = values.astype(jnp.float32)
    scaled = floats * lax.rsqrt(lax.optimization_barrier(jnp.mean(floats * floats, axis=-1, keepdims=True)) + epsilon)
    return (scaled * gain_vec).astype(jnp.bfloat16)

def expert_apply(inputs):
    tokens_in, gate_mat, up_mat, down_mat = inputs
    gate_pre = jnp.dot(tokens_in, gate_mat.T, preferred_element_type=jnp.float32)
    up_pre = jnp.dot(tokens_in, up_mat.T, preferred_element_type=jnp.float32)
    hidden = (jax.nn.silu(gate_pre) * up_pre).astype(jnp.bfloat16)
    return jnp.dot(hidden, down_mat, preferred_element_type=jnp.float32).astype(jnp.bfloat16)

def reference(stream, previous_state, mixer_norm_gain, query_matrix, key_matrix, value_matrix, output_gate_weight, decay_lower_factor, decay_upper_factor, forgetting_boost, head_norm_gain, output_matrix, mixture_norm_gain, expert_gate_weight, expert_up_weight, expert_down_weight, expert_index_table, expert_scores_within, group_probability):
    normed = rms_scaled(stream, mixer_norm_gain)
    queries = (jnp.dot(normed, query_matrix, preferred_element_type=jnp.float32) * KEY_CHANNELS ** (-0.5)).astype(jnp.bfloat16)
    key_rows = jnp.dot(normed, key_matrix, preferred_element_type=jnp.float32).astype(jnp.bfloat16)
    value_rows = jnp.dot(normed, value_matrix, preferred_element_type=jnp.float32).astype(jnp.bfloat16)
    gate_rows = jnp.dot(normed, output_gate_weight, preferred_element_type=jnp.float32).astype(jnp.bfloat16)
    low_rank = jnp.dot(normed, decay_lower_factor, preferred_element_type=jnp.float32).astype(jnp.bfloat16)
    forgetting_logit = jnp.dot(low_rank, decay_upper_factor, preferred_element_type=jnp.float32)
    forgetting_lograte = jax.nn.log_sigmoid(forgetting_logit) / forgetting_softness - forgetting_boost
    factor = jnp.exp(forgetting_lograte).reshape(SEQUENCE_TOTAL, HEAD_TOTAL, KEY_CHANNELS).transpose(0, 2, 1)[..., None]
    state_four = previous_state.reshape(SEQUENCE_TOTAL, KEY_CHANNELS, HEAD_TOTAL, DV)
    key_part = key_rows.astype(jnp.float32).reshape(SEQUENCE_TOTAL, HEAD_TOTAL, KEY_CHANNELS).transpose(0, 2, 1)[..., None]
    value_part = value_rows.astype(jnp.float32).reshape(SEQUENCE_TOTAL, 1, HEAD_TOTAL, DV)
    updated = factor * state_four + key_part * value_part
    query_part = queries.astype(jnp.float32).reshape(SEQUENCE_TOTAL, HEAD_TOTAL, KEY_CHANNELS).transpose(0, 2, 1)
    readout = jnp.einsum('skh,skhv->shv', query_part, updated, precision=lax.Precision.HIGHEST)
    mean_sq = lax.optimization_barrier(jnp.mean(readout * readout, axis=-1, keepdims=True))
    gate_part = jax.nn.silu(gate_rows.astype(jnp.float32).reshape(SEQUENCE_TOTAL, HEAD_TOTAL, DV))
    gated_rows = (readout * lax.rsqrt(mean_sq + epsilon) * head_norm_gain * gate_part).reshape(SEQUENCE_TOTAL, HEAD_TOTAL * DV).astype(jnp.bfloat16)
    blended_tokens = (stream.astype(jnp.float32) + jnp.dot(gated_rows, output_matrix, preferred_element_type=jnp.float32)).astype(jnp.bfloat16)
    normed_two = rms_scaled(blended_tokens, mixture_norm_gain)
    logit_exp = jnp.exp(expert_scores_within)
    weights = logit_exp / lax.optimization_barrier(jnp.sum(logit_exp, axis=-1, keepdims=True)) * group_probability[:, None]
    blocked = expert_index_table.reshape(N_EP, SEQ_DEV * TOPK).astype(jnp.int32)
    one_hot = (blocked[..., None] == jnp.arange(EXPERTS, dtype=jnp.int32)).astype(jnp.int32)
    rank_in = lax.optimization_barrier(jnp.sum(one_hot * (jnp.cumsum(one_hot, axis=1) - 1), axis=-1))
    column = (jnp.arange(N_EP, dtype=jnp.int32)[:, None] * CAP + rank_in).astype(jnp.int32)
    repeated = jnp.broadcast_to(normed_two.reshape(N_EP, SEQ_DEV, 1, D), (N_EP, SEQ_DEV, TOPK, D)).reshape(N_EP, SEQ_DEV * TOPK, D)
    buffer = jnp.zeros((EXPERTS, N_EP * CAP, D), jnp.bfloat16).at[blocked, column].set(repeated)
    results = lax.map(expert_apply, (buffer, expert_gate_weight, expert_up_weight, expert_down_weight))
    picked = results[blocked, column].reshape(SEQUENCE_TOTAL, TOPK, D)
    mixture = lax.optimization_barrier(jnp.sum(weights[..., None] * picked.astype(jnp.float32), axis=1))
    new_stream = (blended_tokens.astype(jnp.float32) + mixture).astype(jnp.bfloat16)
    return (new_stream, updated.reshape(SEQUENCE_TOTAL, KEY_CHANNELS, HEAD_TOTAL * DV))
```

```python
import functools

import jax
import jax.numpy as jnp
from jax import lax
from jax.experimental import pallas as pl
from jax.experimental.pallas import tpu as pltpu
from jax.sharding import PartitionSpec as P

KEY_CHANNELS = 128
DV = 256
W = 128
NX = 4
EPSILON = 1e-06
SOFTNESS = 16.0
MESH = pl.DeviceIdType.MESH
F32 = jnp.float32
BF16 = jnp.bfloat16


def aligned(index, size):
    return pl.ds(pl.multiple_of(index * size, size), size)


def kernel(
    ec,
    tc,
    nx,
    cap,
    stream_h,
    state_h,
    gain1_h,
    query_h,
    key_h,
    value_h,
    gate_h,
    lower_h,
    upper_h,
    boost_h,
    hgain_h,
    wo_h,
    gain2_h,
    eg_h,
    eu_h,
    ed_h,
    ids_h,
    scores_h,
    prob_h,
    out_h,
    newstate_h,
    stream,
    state,
    gain1,
    wraw,
    wcat,
    lower,
    upper,
    boost,
    hgain,
    wo,
    gain2,
    egu,
    ed,
    ids,
    scores,
    prob,
    xin,
    pbuf,
    pin,
    ssb,
    obuf,
    oin,
    dbuf,
    rin,
    xg,
    w4,
    wdp,
    hin,
    rbuf,
    retin,
    ro,
    outv,
    factor_t,
    comb,
    disp,
    lsem,
    ssem,
    rsem,
    xsem,
    ysem,
):
    ep = lax.axis_index("ep")
    tp = lax.axis_index("tp")
    zc = ec // 2
    ny = tc // nx
    z = ep // 2
    core = ep % 2
    y = tp // nx
    x = tp % nx
    heads_before = tp * W // DV
    half = tp % (DV // W)
    seqs, width = stream.shape
    units = eg_h.shape[1]
    ff = units * tc
    slots = ec * cap

    barrier = pltpu.get_barrier_semaphore()

    def greet_ep(i, carry):
        pl.semaphore_signal(
            barrier, inc=1, device_id=((ep + i) % ec, tp), device_id_type=MESH
        )
        return carry

    def greet_tp(i, carry):
        pl.semaphore_signal(
            barrier, inc=1, device_id=(ep, (tp + i) % tc), device_id_type=MESH
        )
        return carry

    lax.fori_loop(1, ec, greet_ep, 0)
    lax.fori_loop(1, tc, greet_tp, 0)

    copies = {}

    def load(name, src, dst):
        cp = pltpu.make_async_copy(src, dst, lsem.at[len(copies)])
        cp.start()
        copies[name] = cp

    head_cols = aligned(heads_before, W)
    load("stream", stream_h, stream)
    load("gain1", gain1_h, gain1)
    load("wq", query_h.at[:, head_cols], wraw.at[:, pl.ds(0, W)])
    load("wk", key_h.at[:, head_cols], wraw.at[:, pl.ds(W, W)])
    load("wv", value_h, wraw.at[:, pl.ds(2 * W, W)])
    load("wg", gate_h, wraw.at[:, pl.ds(3 * W, W)])
    load("lower", lower_h, lower)
    load("upper", upper_h.at[:, head_cols], upper)
    load("boost", boost_h.at[:, head_cols], boost)
    load("state", state_h, state)
    load("ids", ids_h, ids)
    load("scores", scores_h, scores)
    load("prob", prob_h, prob)
    load("hgain", hgain_h, hgain)
    load("wo", wo_h, wo)
    load("gain2", gain2_h, gain2)
    load("eg", eg_h.at[0], egu.at[0])
    load("eu", eu_h.at[0], egu.at[1])
    load("ed", ed_h.at[0], ed)

    def arrive(*names):
        for name in names:
            copies[name].wait()

    def settle(ref, sem):
        pltpu.make_async_copy(ref, ref, sem).wait()

    arrive("gain1", "wq", "wk", "wv", "wg")
    gain_row = gain1[:, aligned(ep, W)]
    gain_col = jnp.transpose(jnp.broadcast_to(gain_row, (W, W)))
    gain_wide = jnp.concatenate([gain_col] * 4, axis=1)
    wcat[aligned(core, W), :] = (wraw[...].astype(F32) * gain_wide).astype(BF16)

    arrive("stream")
    rows = stream[...].astype(F32)
    scale1 = lax.rsqrt(jnp.mean(rows * rows, axis=1, keepdims=True) + EPSILON)
    normed = (rows * scale1 * gain1[...]).astype(BF16)

    pl.semaphore_wait(barrier, ec + tc - 2)

    def send(src, dst, sent, received, device):
        pltpu.make_async_remote_copy(
            src_ref=src,
            dst_ref=dst,
            send_sem=sent,
            recv_sem=received,
            device_id=device,
            device_id_type=MESH,
        ).start()

    half_rows = wcat.at[aligned(core, W)]
    send(half_rows, half_rows, ssem.at[0], rsem.at[0], (ep + 1 - 2 * core, tp))
    chip_width = 2 * W

    def send_x(to):
        send(
            stream.at[:, aligned(to, chip_width)],
            xin.at[aligned(z, seqs)],
            ssem.at[1],
            xsem.at[z],
            (to * 2 + core, tp),
        )

    send_x((z + zc // 2) % zc)

    def send_x_pair(i, carry):
        d = zc // 2 - i
        send_x((z + d) % zc)
        send_x((z + zc - d) % zc)
        return carry

    lax.fori_loop(1, zc // 2, send_x_pair, 0)

    arrive("lower", "upper", "boost")
    low = lax.dot_general(
        normed, lower[...], (((1,), (1,)), ((), ())), preferred_element_type=F32
    ).astype(BF16)
    logit = jnp.dot(low, upper[...], preferred_element_type=F32)
    lograte = jax.nn.log_sigmoid(logit) / SOFTNESS - boost[...]
    factor_t[...] = jnp.transpose(jnp.exp(lograte))

    arrive("ids", "scores", "prob")
    lane = lax.broadcasted_iota(jnp.int32, (seqs, slots), 1)
    mine = (lane // cap).astype(F32)
    diagonal = lax.broadcasted_iota(jnp.int32, (seqs, seqs), 0) == lax.broadcasted_iota(
        jnp.int32, (seqs, seqs), 1
    )

    def column(row):
        square = jnp.where(diagonal, jnp.broadcast_to(row, (seqs, seqs)), 0.0)
        return jnp.sum(square, axis=1, keepdims=True)

    first = jnp.where(column(ids[0:1, :].astype(F32)) == mine, 1.0, 0.0)
    second = jnp.where(column(ids[1:2, :].astype(F32)) == mine, 1.0, 0.0)
    either = first + second
    before = jnp.where(
        lax.broadcasted_iota(jnp.int32, (seqs, seqs), 1)
        < lax.broadcasted_iota(jnp.int32, (seqs, seqs), 0),
        1.0,
        0.0,
    )
    earlier = jnp.dot(
        before.astype(BF16), either.astype(BF16), preferred_element_type=F32
    )
    chosen = jnp.where(jnp.abs(earlier - (lane % cap).astype(F32)) < 0.5, either, 0.0)
    disp[...] = jnp.transpose(chosen).astype(BF16)
    raised = jnp.exp(scores[...])
    weights = raised / jnp.sum(raised, axis=0, keepdims=True) * prob[...]
    comb[...] = chosen * (first * column(weights[0:1, :]) + second * column(weights[1:2, :]))

    pltpu.make_async_remote_copy(
        src_ref=half_rows,
        dst_ref=wcat.at[aligned(1 - core, W)],
        send_sem=ssem.at[0],
        recv_sem=rsem.at[0],
        device_id=(ep + 1 - 2 * core, tp),
        device_id_type=MESH,
    ).wait()

    pin[aligned(z, seqs), :] = jnp.dot(
        stream[:, aligned(z, chip_width)], wcat[...], preferred_element_type=F32
    ).astype(BF16)

    def answer(to):
        settle(xin.at[aligned(to, seqs)], xsem.at[to])
        pbuf[aligned(to, seqs), :] = jnp.dot(
            xin[aligned(to, seqs), :], wcat[...], preferred_element_type=F32
        ).astype(BF16)
        send(
            pbuf.at[aligned(to, seqs)],
            pin.at[aligned(z, seqs)],
            ssem.at[2],
            rsem.at[1],
            (to * 2 + core, tp),
        )

    def answer_pair(d, carry):
        answer((z + d) % zc)
        answer((z + zc - d) % zc)
        return carry

    lax.fori_loop(1, zc // 2, answer_pair, 0)
    answer((z + zc // 2) % zc)

    arrive("state")
    for s in range(seqs):
        state[s] = state[s] * factor_t[:, s : s + 1]

    arrive("gain2", "eg", "eu")
    for which in range(2):
        scaled = (egu[which].astype(F32) * gain2[...]).astype(BF16)
        for copy in range(4):
            w4[pl.ds((which * 4 + copy) * units, units), :] = scaled
    arrive("ed")
    for g in range(4):
        for block in range(ff // units):
            source = block // 4 * 4 + (block % 4 - g) % 4
            wdp[g, pl.ds(block * units, units), :] = ed[pl.ds(source * units, units), :]
    arrive("hgain", "wo")

    settle(pin.at[pl.ds(0, (zc - 1) * seqs)], rsem.at[1])
    total = pin[pl.ds(0, seqs), :].astype(F32)
    for i in range(1, zc):
        total = total + pin[pl.ds(i * seqs, seqs), :].astype(F32)
    total = total * scale1

    query_t = jnp.transpose(total[:, :W] * KEY_CHANNELS**-0.5)
    key_t = jnp.transpose(total[:, W : 2 * W])
    value_rows = total[:, 2 * W : 3 * W]
    gate_rows = total[:, 3 * W :]
    for s in range(seqs):
        fresh = state[s] + key_t[:, s : s + 1] * value_rows[s : s + 1, :]
        state[s] = fresh
        ro[s : s + 1, :] = jnp.sum(query_t[:, s : s + 1] * fresh, axis=0, keepdims=True)
    readout = ro[...]
    squares = jnp.sum(readout * readout, axis=1, keepdims=True)
    ssb[0] = jnp.broadcast_to(squares, (seqs, W))
    partner = tp + 1 - 2 * half
    gated = (
        readout * hgain[:, aligned(half, W)] * (gate_rows * jax.nn.sigmoid(gate_rows))
    ).astype(BF16)
    exchange = pltpu.make_async_remote_copy(
        src_ref=ssb.at[0],
        dst_ref=ssb.at[1],
        send_sem=ssem.at[3],
        recv_sem=rsem.at[2],
        device_id=(ep, partner),
        device_id_type=MESH,
    )
    exchange.start()
    partial = jnp.dot(gated, wo[...], preferred_element_type=F32)
    store_state = pltpu.make_async_copy(state, newstate_h, lsem.at[len(copies)])
    store_state.start()
    exchange.wait()
    head_scale = lax.rsqrt((squares + ssb[1, :, 0:1]) / DV + EPSILON)
    obuf[...] = (partial * head_scale).astype(BF16)

    def send_o(i, carry):
        to = (tp + i) % tc
        send(obuf.at[:, aligned(to, W)], oin.at[tp], ssem.at[4], rsem.at[3], (ep, to))
        return carry

    lax.fori_loop(1, tc, send_o, 0)
    oin[tp] = obuf[:, aligned(tp, W)]
    settle(oin.at[pl.ds(0, tc - 1)], rsem.at[3])
    mixed = stream[:, aligned(tp, W)].astype(F32)
    summed = oin[0].astype(F32)
    for i in range(1, tc):
        summed = summed + oin[i].astype(F32)
    mixed = (mixed + summed).astype(BF16)

    dbuf[...] = jnp.dot(disp[...], mixed, preferred_element_type=F32).astype(BF16)

    def send_d(i, carry):
        to = (ep + i) % ec
        send(
            dbuf.at[aligned(to, cap)],
            rin.at[aligned(ep, cap)],
            ssem.at[5],
            rsem.at[4],
            (to, tp),
        )
        return carry

    lax.fori_loop(1, ec, send_d, 0)
    own = lax.broadcasted_iota(jnp.int32, (slots, W), 0) // cap == ep
    settle(rin.at[pl.ds(0, (ec - 1) * cap)], rsem.at[4])
    xg[tp] = jnp.where(own, dbuf[...].astype(F32), rin[...].astype(F32)).astype(BF16)

    def send_y(i, carry):
        to = ((y + i) % ny) * nx + x
        send(xg.at[tp], xg.at[tp], ssem.at[6], ysem.at[y], (ep, to))
        return carry

    lax.fori_loop(1, ny, send_y, 0)

    def pass_x(block):
        for i in range(1, nx):
            to = y * nx + (x + i) % nx
            send(xg.at[block], xg.at[block], ssem.at[7], rsem.at[5], (ep, to))

    pass_x(tp)

    def forward(i, carry):
        from_y = (y + i) % ny
        block = from_y * nx + x
        settle(xg.at[block], ysem.at[from_y])
        pass_x(block)
        return carry

    lax.fori_loop(1, ny, forward, 0)
    settle(xg.at[pl.ds(0, (nx - 1) * ny)], rsem.at[5])

    expert_rows = jnp.concatenate([xg[i] for i in range(tc)], axis=1)
    square = jnp.zeros((slots, W), F32)
    for i in range(tc):
        piece = xg[i].astype(F32)
        square = square + piece * piece
    scale2 = lax.rsqrt(jnp.sum(square, axis=1, keepdims=True) / width + EPSILON)
    both = lax.dot_general(
        expert_rows, w4[...], (((1,), (1,)), ((), ())), preferred_element_type=F32
    )
    gate_pre = both[:, : 4 * units] * scale2
    up_pre = both[:, 4 * units :] * scale2
    hidden = gate_pre * jax.nn.sigmoid(gate_pre) * up_pre
    group = slots // 4
    quarter = lax.broadcasted_iota(jnp.int32, (group, W), 1) // units
    tile = jnp.zeros((group, W), F32)
    for g in range(4):
        tile = jnp.where(
            quarter == (g + tp % 4) % 4, hidden[g * group : (g + 1) * group, :], tile
        )
    hin[tp] = tile.astype(BF16)

    def send_h(i, carry):
        to = (tp + i) % tc
        send(hin.at[tp], hin.at[tp], ssem.at[8], rsem.at[6], (ep, to))
        return carry

    lax.fori_loop(1, tc, send_h, 0)
    settle(hin.at[pl.ds(0, tc - 1)], rsem.at[6])

    for g in range(4):
        pieces = []
        for a in range(tc // 4):
            piece = hin[4 * a].astype(F32)
            for b in range(1, 4):
                piece = jnp.where(
                    quarter == (g + b) % 4, hin[4 * a + b].astype(F32), piece
                )
            pieces.append(piece.astype(BF16))
        rbuf[pl.ds(g * group, group), :] = jnp.dot(
            jnp.concatenate(pieces, axis=1), wdp[g], preferred_element_type=F32
        ).astype(BF16)

    def send_r(i, carry):
        to = (ep + i) % ec
        send(
            rbuf.at[aligned(to, cap)],
            retin.at[aligned(ep, cap)],
            ssem.at[9],
            rsem.at[7],
            (to, tp),
        )
        return carry

    lax.fori_loop(1, ec, send_r, 0)
    weight_high = comb[...].astype(BF16)
    weight_low = (comb[...] - weight_high.astype(F32)).astype(BF16)
    settle(retin.at[pl.ds(0, (ec - 1) * cap)], rsem.at[7])
    back = jnp.where(own, rbuf[...].astype(F32), retin[...].astype(F32)).astype(BF16)
    mixture = jnp.dot(weight_high, back, preferred_element_type=F32) + jnp.dot(
        weight_low, back, preferred_element_type=F32
    )
    outv[...] = (mixed.astype(F32) + mixture).astype(BF16)
    store_out = pltpu.make_async_copy(outv, out_h, lsem.at[len(copies) + 1])
    store_out.start()

    settle(xin.at[pl.ds(0, (zc - 1) * seqs)], ssem.at[1])
    settle(pbuf.at[pl.ds(0, (zc - 1) * seqs)], ssem.at[2])
    settle(oin.at[pl.ds(0, tc - 1)], ssem.at[4])
    settle(rin.at[pl.ds(0, (ec - 1) * cap)], ssem.at[5])
    settle(xg.at[pl.ds(0, ny - 1)], ssem.at[6])
    settle(xg.at[pl.ds(0, (nx - 1) * ny)], ssem.at[7])
    settle(hin.at[pl.ds(0, tc - 1)], ssem.at[8])
    settle(rin.at[pl.ds(0, (ec - 1) * cap)], ssem.at[9])
    store_state.wait()
    store_out.wait()


def on_device(ec, tc, nx, *args):
    (
        stream,
        previous_state,
        mixer_norm_gain,
        query_matrix,
        key_matrix,
        value_matrix,
        output_gate_weight,
        decay_lower_factor,
        decay_upper_factor,
        forgetting_boost,
        head_norm_gain,
        output_matrix,
        mixture_norm_gain,
        expert_gate_weight,
        expert_up_weight,
        expert_down_weight,
        expert_index_table,
        expert_scores_within,
        group_probability,
    ) = args
    seqs, width = stream.shape
    cap = 2 * seqs * expert_index_table.shape[1] // ec
    slots = ec * cap
    units = expert_gate_weight.shape[1]
    ff = expert_down_weight.shape[1]
    zc = ec // 2
    operands = (
        stream,
        previous_state,
        mixer_norm_gain.reshape(1, width),
        query_matrix,
        key_matrix,
        value_matrix,
        output_gate_weight,
        decay_lower_factor.T,
        decay_upper_factor,
        forgetting_boost,
        head_norm_gain.reshape(1, DV),
        output_matrix,
        mixture_norm_gain.reshape(1, width),
        expert_gate_weight,
        expert_up_weight,
        expert_down_weight,
        expert_index_table.T,
        expert_scores_within.T,
        group_probability.reshape(1, seqs),
    )
    v = pltpu.VMEM
    scratch = [
        v((seqs, width), BF16),
        v(previous_state.shape, F32),
        v((1, width), F32),
        v((W, 4 * W), BF16),
        v((2 * W, 4 * W), BF16),
        v(decay_lower_factor.shape[::-1], BF16),
        v((decay_upper_factor.shape[0], W), BF16),
        v((seqs, W), F32),
        v((1, DV), F32),
        v(output_matrix.shape, BF16),
        v((1, width), F32),
        v((2, units, width), BF16),
        v((ff, W), BF16),
        v(expert_index_table.shape[::-1], jnp.int32),
        v(expert_scores_within.shape[::-1], F32),
        v((1, seqs), F32),
        v((zc * seqs, 2 * W), BF16),
        v((zc * seqs, 4 * W), BF16),
        v((zc * seqs, 4 * W), BF16),
        v((2, seqs, W), F32),
        v((seqs, width), BF16),
        v((tc, seqs, W), BF16),
        v((slots, W), BF16),
        v((slots, W), BF16),
        v((tc, slots, W), BF16),
        v((8 * units, width), BF16),
        v((4, ff, W), BF16),
        v((tc, slots // 4, W), BF16),
        v((slots, W), BF16),
        v((slots, W), BF16),
        v((seqs, W), F32),
        v((seqs, W), BF16),
        v((W, seqs), F32),
        v((seqs, slots), F32),
        v((slots, seqs), BF16),
        pltpu.SemaphoreType.DMA((21,)),
        pltpu.SemaphoreType.DMA((10,)),
        pltpu.SemaphoreType.DMA((8,)),
        pltpu.SemaphoreType.DMA((zc,)),
        pltpu.SemaphoreType.DMA((tc // nx,)),
    ]
    hbm = pl.BlockSpec(memory_space=pltpu.HBM)
    return pl.pallas_call(
        functools.partial(kernel, ec, tc, nx, cap),
        out_shape=(
            jax.ShapeDtypeStruct((seqs, W), BF16),
            jax.ShapeDtypeStruct(previous_state.shape, F32),
        ),
        in_specs=[hbm] * len(operands),
        out_specs=(hbm, hbm),
        scratch_shapes=scratch,
        compiler_params=pltpu.CompilerParams(
            collective_id=0, has_side_effects=True, vmem_limit_bytes=67043328
        ),
        name="layer",
    )(*operands)


def solution(mesh):
    ec, tc = mesh.shape["ep"], mesh.shape["tp"]
    placed = (
        P("ep", None),
        P("ep", None, "tp"),
        P(),
        P("ep", None),
        P("ep", None),
        P("ep", "tp"),
        P("ep", "tp"),
        P(),
        P(),
        P("ep", None),
        P(),
        P("tp", None),
        P(),
        P("ep", "tp", None),
        P("ep", "tp", None),
        P("ep", None, "tp"),
        P("ep", None),
        P("ep", None),
        P("ep"),
    )
    return jax.shard_map(
        functools.partial(on_device, ec, tc, min(NX, tc // 2)),
        mesh=mesh,
        in_specs=placed,
        out_specs=(P("ep", "tp"), P("ep", None, "tp")),
        check_vma=False,
    )
```

```python
import functools

import jax
import jax.numpy as jnp
from jax import lax
from jax.experimental import pallas as pl
from jax.experimental.pallas import tpu as pltpu
from jax.sharding import PartitionSpec as P

KEY_CHANNELS = 128
DV = 256
W = 128
NX = 4
EPSILON = 1e-06
SOFTNESS = 16.0
MESH = pl.DeviceIdType.MESH
F32 = jnp.float32
BF16 = jnp.bfloat16


def aligned(index, size):
    return pl.ds(pl.multiple_of(index * size, size), size)


def kernel(
    ec,
    tc,
    nx,
    cap,
    stream_h,
    state_h,
    gain1_h,
    query_h,
    key_h,
    value_h,
    gate_h,
    lower_h,
    upper_h,
    boost_h,
    hgain_h,
    wo_h,
    gain2_h,
    eg_h,
    eu_h,
    ed_h,
    ids_h,
    scores_h,
    prob_h,
    out_h,
    newstate_h,
    stream,
    state,
    gain1,
    wraw,
    wcat,
    lower,
    upper,
    boost,
    hgain,
    wo,
    gain2,
    egu,
    ed,
    ids,
    scores,
    prob,
    xin,
    pbuf,
    pin,
    qbuf,
    qin,
    qkb,
    ssb,
    obuf,
    oin,
    dbuf,
    rin,
    xg,
    w4,
    wdp,
    hin,
    rbuf,
    retin,
    ro,
    outv,
    factor_t,
    comb,
    disp,
    lsem,
    ssem,
    rsem,
    xsem,
    bsem,
):
    ep = lax.axis_index("ep")
    tp = lax.axis_index("tp")
    zc = ec // 2
    ny = tc // nx
    z = ep // 2
    core = ep % 2
    y = tp // nx
    x = tp % nx
    heads_before = tp * W // DV
    half = tp % (DV // W)
    seqs, width = stream.shape
    units = eg_h.shape[1]
    ff = units * tc
    slots = ec * cap

    barrier = pltpu.get_barrier_semaphore()

    def greet_ep(i, carry):
        pl.semaphore_signal(
            barrier, inc=1, device_id=((ep + i) % ec, tp), device_id_type=MESH
        )
        return carry

    def greet_tp(i, carry):
        pl.semaphore_signal(
            barrier, inc=1, device_id=(ep, (tp + i) % tc), device_id_type=MESH
        )
        return carry

    lax.fori_loop(1, ec, greet_ep, 0)
    lax.fori_loop(1, tc, greet_tp, 0)

    copies = {}

    def load(name, src, dst):
        cp = pltpu.make_async_copy(src, dst, lsem.at[len(copies)])
        cp.start()
        copies[name] = cp

    head_cols = aligned(heads_before, W)
    load("stream", stream_h, stream)
    load("gain1", gain1_h, gain1)
    load("wq", query_h.at[:, head_cols], wraw.at[:, pl.ds(0, W)])
    load("wk", key_h.at[:, head_cols], wraw.at[:, pl.ds(W, W)])
    load("wv", value_h, wraw.at[:, pl.ds(2 * W, W)])
    load("wg", gate_h, wraw.at[:, pl.ds(3 * W, W)])
    load("lower", lower_h, lower)
    load("upper", upper_h.at[:, head_cols], upper)
    load("boost", boost_h.at[:, head_cols], boost)
    load("state", state_h, state)
    load("ids", ids_h, ids)
    load("scores", scores_h, scores)
    load("prob", prob_h, prob)
    load("hgain", hgain_h, hgain)
    load("wo", wo_h, wo)
    load("gain2", gain2_h, gain2)
    load("eg", eg_h.at[0], egu.at[0])
    load("eu", eu_h.at[0], egu.at[1])
    load("ed", ed_h.at[0], ed)

    def arrive(*names):
        for name in names:
            copies[name].wait()

    def settle(ref, sem):
        pltpu.make_async_copy(ref, ref, sem).wait()

    arrive("gain1", "wq", "wk", "wv", "wg")
    gain_row = gain1[:, aligned(ep, W)]
    gain_col = jnp.transpose(jnp.broadcast_to(gain_row, (W, W)))
    first_half = half == 0
    shared = jnp.where(
        first_half, wraw[:, :W].astype(F32), wraw[:, W : 2 * W].astype(F32)
    )
    wcat[aligned(core, W), :W] = (shared * gain_col).astype(BF16)
    gain_wide = jnp.concatenate([gain_col] * 2, axis=1)
    wcat[aligned(core, W), W:] = (wraw[:, 2 * W :].astype(F32) * gain_wide).astype(BF16)

    arrive("stream")
    rows = stream[...].astype(F32)
    scale1 = lax.rsqrt(jnp.mean(rows * rows, axis=1, keepdims=True) + EPSILON)
    normed = (rows * scale1 * gain1[...]).astype(BF16)

    pl.semaphore_wait(barrier, ec + tc - 2)

    def send(src, dst, sent, received, device):
        pltpu.make_async_remote_copy(
            src_ref=src,
            dst_ref=dst,
            send_sem=sent,
            recv_sem=received,
            device_id=device,
            device_id_type=MESH,
        ).start()

    half_rows = wcat.at[aligned(core, W)]
    send(half_rows, half_rows, ssem.at[0], rsem.at[0], (ep + 1 - 2 * core, tp))
    chip_width = 2 * W

    def send_x(to):
        send(
            stream.at[:, aligned(to, chip_width)],
            xin.at[aligned(z, seqs)],
            ssem.at[1],
            xsem.at[z],
            (to * 2 + core, tp),
        )

    send_x((z + zc // 2) % zc)

    def send_x_pair(i, carry):
        d = zc // 2 - i
        send_x((z + d) % zc)
        send_x((z + zc - d) % zc)
        return carry

    lax.fori_loop(1, zc // 2, send_x_pair, 0)

    arrive("lower", "upper", "boost")
    low = lax.dot_general(
        normed, lower[...], (((1,), (1,)), ((), ())), preferred_element_type=F32
    ).astype(BF16)
    logit = jnp.dot(low, upper[...], preferred_element_type=F32)
    lograte = jax.nn.log_sigmoid(logit) / SOFTNESS - boost[...]
    factor_t[...] = jnp.transpose(jnp.exp(lograte))

    arrive("ids", "scores", "prob")
    lane = lax.broadcasted_iota(jnp.int32, (seqs, slots), 1)
    mine = (lane // cap).astype(F32)
    diagonal = lax.broadcasted_iota(jnp.int32, (seqs, seqs), 0) == lax.broadcasted_iota(
        jnp.int32, (seqs, seqs), 1
    )

    def column(row):
        square = jnp.where(diagonal, jnp.broadcast_to(row, (seqs, seqs)), 0.0)
        return jnp.sum(square, axis=1, keepdims=True)

    first = jnp.where(column(ids[0:1, :].astype(F32)) == mine, 1.0, 0.0)
    second = jnp.where(column(ids[1:2, :].astype(F32)) == mine, 1.0, 0.0)
    either = first + second
    before = jnp.where(
        lax.broadcasted_iota(jnp.int32, (seqs, seqs), 1)
        < lax.broadcasted_iota(jnp.int32, (seqs, seqs), 0),
        1.0,
        0.0,
    )
    earlier = jnp.dot(
        before.astype(BF16), either.astype(BF16), preferred_element_type=F32
    )
    chosen = jnp.where(jnp.abs(earlier - (lane % cap).astype(F32)) < 0.5, either, 0.0)
    disp[...] = jnp.transpose(chosen).astype(BF16)
    raised = jnp.exp(scores[...])
    weights = raised / jnp.sum(raised, axis=0, keepdims=True) * prob[...]
    comb[...] = chosen * (first * column(weights[0:1, :]) + second * column(weights[1:2, :]))

    pltpu.make_async_remote_copy(
        src_ref=half_rows,
        dst_ref=wcat.at[aligned(1 - core, W)],
        send_sem=ssem.at[0],
        recv_sem=rsem.at[0],
        device_id=(ep + 1 - 2 * core, tp),
        device_id_type=MESH,
    ).wait()

    xin[aligned(z, seqs), :] = stream[:, aligned(z, chip_width)]

    qin[aligned(z, seqs), :] = jnp.dot(
        xin[aligned(z, seqs), :], wcat[:, :W], preferred_element_type=F32
    ).astype(BF16)

    def send_q(to):
        send(
            qbuf.at[aligned(to, seqs)],
            qin.at[aligned(z, seqs)],
            ssem.at[10],
            rsem.at[8],
            (to * 2 + core, tp),
        )

    def answer_pair(d, carry):
        above = (z + d) % zc
        below = (z + zc - d) % zc
        settle(xin.at[aligned(above, seqs)], xsem.at[above])
        settle(xin.at[aligned(below, seqs)], xsem.at[below])
        pair = jnp.concatenate(
            [xin[aligned(above, seqs), :], xin[aligned(below, seqs), :]], axis=0
        )
        sums = jnp.dot(pair, wcat[:, :W], preferred_element_type=F32).astype(BF16)
        qbuf[aligned(above, seqs), :] = sums[:seqs]
        qbuf[aligned(below, seqs), :] = sums[seqs:]
        send_q(above)
        send_q(below)
        return carry

    lax.fori_loop(1, zc // 2, answer_pair, 0)
    across = (z + zc // 2) % zc
    settle(xin.at[aligned(across, seqs)], xsem.at[across])
    qbuf[aligned(across, seqs), :] = jnp.dot(
        xin[aligned(across, seqs), :], wcat[:, :W], preferred_element_type=F32
    ).astype(BF16)
    send_q(across)

    pbuf[...] = jnp.dot(xin[...], wcat[:, W:], preferred_element_type=F32).astype(BF16)

    def send_p(to):
        send(
            pbuf.at[aligned(to, seqs)],
            pin.at[aligned(z, seqs)],
            ssem.at[2],
            rsem.at[1],
            (to * 2 + core, tp),
        )

    send_p(across)

    def send_p_pair(i, carry):
        d = zc // 2 - i
        send_p((z + d) % zc)
        send_p((z + zc - d) % zc)
        return carry

    lax.fori_loop(1, zc // 2, send_p_pair, 0)
    pin[aligned(z, seqs), :] = pbuf[aligned(z, seqs), :]

    arrive("state")
    for s in range(seqs):
        state[s] = state[s] * factor_t[:, s : s + 1]

    arrive("gain2", "eg", "eu")
    for which in range(2):
        scaled = (egu[which].astype(F32) * gain2[...]).astype(BF16)
        for copy in range(4):
            w4[pl.ds((which * 4 + copy) * units, units), :] = scaled
    arrive("ed")
    for g in range(4):
        for block in range(ff // units):
            source = block // 4 * 4 + (block % 4 - g) % 4
            wdp[g, pl.ds(block * units, units), :] = ed[pl.ds(source * units, units), :]
    arrive("hgain", "wo")

    settle(qin.at[pl.ds(0, (zc - 1) * seqs)], rsem.at[8])
    own_sum = qin[pl.ds(0, seqs), :].astype(F32)
    for i in range(1, zc):
        own_sum = own_sum + qin[pl.ds(i * seqs, seqs), :].astype(F32)
    partner = tp + 1 - 2 * half
    qkb[0] = own_sum * scale1
    swap = pltpu.make_async_remote_copy(
        src_ref=qkb.at[0],
        dst_ref=qkb.at[1],
        send_sem=ssem.at[11],
        recv_sem=rsem.at[9],
        device_id=(ep, partner),
        device_id_type=MESH,
    )
    swap.start()

    settle(pin.at[pl.ds(0, (zc - 1) * seqs)], rsem.at[1])
    total = pin[pl.ds(0, seqs), :].astype(F32)
    for i in range(1, zc):
        total = total + pin[pl.ds(i * seqs, seqs), :].astype(F32)
    total = total * scale1
    swap.wait()

    query_rows = jnp.where(first_half, qkb[0], qkb[1])
    key_rows = jnp.where(first_half, qkb[1], qkb[0])
    query_t = jnp.transpose(query_rows * KEY_CHANNELS**-0.5)
    key_t = jnp.transpose(key_rows)
    value_rows = total[:, :W]
    gate_rows = total[:, W:]
    for s in range(seqs):
        fresh = state[s] + key_t[:, s : s + 1] * value_rows[s : s + 1, :]
        state[s] = fresh
        ro[s : s + 1, :] = jnp.sum(query_t[:, s : s + 1] * fresh, axis=0, keepdims=True)
    readout = ro[...]
    squares = jnp.sum(readout * readout, axis=1, keepdims=True)
    ssb[0] = jnp.broadcast_to(squares, (seqs, W))
    gated = (
        readout * hgain[:, aligned(half, W)] * (gate_rows * jax.nn.sigmoid(gate_rows))
    ).astype(BF16)
    exchange = pltpu.make_async_remote_copy(
        src_ref=ssb.at[0],
        dst_ref=ssb.at[1],
        send_sem=ssem.at[3],
        recv_sem=rsem.at[2],
        device_id=(ep, partner),
        device_id_type=MESH,
    )
    exchange.start()
    partial = jnp.dot(gated, wo[...], preferred_element_type=F32)
    store_state = pltpu.make_async_copy(state, newstate_h, lsem.at[len(copies)])
    store_state.start()
    exchange.wait()
    head_scale = lax.rsqrt((squares + ssb[1, :, 0:1]) / DV + EPSILON)
    obuf[...] = (partial * head_scale).astype(BF16)

    def send_o(i, carry):
        to = (tp + i) % tc
        send(obuf.at[:, aligned(to, W)], oin.at[tp], ssem.at[4], rsem.at[3], (ep, to))
        return carry

    lax.fori_loop(1, tc, send_o, 0)
    oin[tp] = obuf[:, aligned(tp, W)]
    settle(oin.at[pl.ds(0, tc - 1)], rsem.at[3])
    mixed = stream[:, aligned(tp, W)].astype(F32)
    summed = oin[0].astype(F32)
    for i in range(1, tc):
        summed = summed + oin[i].astype(F32)
    mixed = (mixed + summed).astype(BF16)

    dbuf[...] = jnp.dot(disp[...], mixed, preferred_element_type=F32).astype(BF16)

    def send_d(i, carry):
        to = (ep + i) % ec
        send(
            dbuf.at[aligned(to, cap)],
            rin.at[aligned(ep, cap)],
            ssem.at[5],
            rsem.at[4],
            (to, tp),
        )
        return carry

    lax.fori_loop(1, ec, send_d, 0)
    own = lax.broadcasted_iota(jnp.int32, (slots, W), 0) // cap == ep
    settle(rin.at[pl.ds(0, (ec - 1) * cap)], rsem.at[4])
    xg[tp] = jnp.where(own, dbuf[...].astype(F32), rin[...].astype(F32)).astype(BF16)

    def send_y(i, carry):
        to = ((y + i) % ny) * nx + x
        send(xg.at[tp], xg.at[tp], ssem.at[6], bsem.at[tp], (ep, to))
        return carry

    lax.fori_loop(1, ny, send_y, 0)

    def pass_x(block):
        for i in range(1, nx):
            to = y * nx + (x + i) % nx
            send(xg.at[block], xg.at[block], ssem.at[7], bsem.at[block], (ep, to))

    pass_x(tp)

    def from_row(i):
        return (y + ny + (2 * (i % 2) - 1) * ((i + 1) // 2)) % ny

    def forward(i, carry):
        block = from_row(i) * nx + x
        settle(xg.at[block], bsem.at[block])
        pass_x(block)
        return carry

    lax.fori_loop(1, ny, forward, 0)

    def products(i, carry):
        both, square = carry
        row = from_row(i) * nx
        for k in range(1, nx):
            block = row + (x + k) % nx
            settle(xg.at[block], bsem.at[block])
        pieces = [xg[row + k] for k in range(nx)]
        for piece in pieces:
            floats = piece.astype(F32)
            square = square + floats * floats
        both = both + lax.dot_general(
            jnp.concatenate(pieces, axis=1),
            w4[:, aligned(from_row(i), nx * W)],
            (((1,), (1,)), ((), ())),
            preferred_element_type=F32,
        )
        return both, square

    both, square = lax.fori_loop(
        0,
        ny,
        products,
        (jnp.zeros((slots, 8 * units), F32), jnp.zeros((slots, W), F32)),
    )
    scale2 = lax.rsqrt(jnp.sum(square, axis=1, keepdims=True) / width + EPSILON)
    gate_pre = both[:, : 4 * units] * scale2
    up_pre = both[:, 4 * units :] * scale2
    hidden = gate_pre * jax.nn.sigmoid(gate_pre) * up_pre
    group = slots // 4
    quarter = lax.broadcasted_iota(jnp.int32, (group, W), 1) // units
    tile = jnp.zeros((group, W), F32)
    for g in range(4):
        tile = jnp.where(
            quarter == (g + tp % 4) % 4, hidden[g * group : (g + 1) * group, :], tile
        )
    hin[tp] = tile.astype(BF16)

    def send_h(i, carry):
        to = (tp + i) % tc
        send(hin.at[tp], hin.at[tp], ssem.at[8], rsem.at[6], (ep, to))
        return carry

    lax.fori_loop(1, tc, send_h, 0)
    settle(hin.at[pl.ds(0, tc - 1)], rsem.at[6])

    for g in range(4):
        pieces = []
        for a in range(tc // 4):
            piece = hin[4 * a].astype(F32)
            for b in range(1, 4):
                piece = jnp.where(
                    quarter == (g + b) % 4, hin[4 * a + b].astype(F32), piece
                )
            pieces.append(piece.astype(BF16))
        rbuf[pl.ds(g * group, group), :] = jnp.dot(
            jnp.concatenate(pieces, axis=1), wdp[g], preferred_element_type=F32
        ).astype(BF16)

    def send_r(i, carry):
        to = (ep + i) % ec
        send(
            rbuf.at[aligned(to, cap)],
            retin.at[aligned(ep, cap)],
            ssem.at[9],
            rsem.at[7],
            (to, tp),
        )
        return carry

    lax.fori_loop(1, ec, send_r, 0)
    weight_high = comb[...].astype(BF16)
    weight_low = (comb[...] - weight_high.astype(F32)).astype(BF16)
    settle(retin.at[pl.ds(0, (ec - 1) * cap)], rsem.at[7])
    back = jnp.where(own, rbuf[...].astype(F32), retin[...].astype(F32)).astype(BF16)
    mixture = jnp.dot(weight_high, back, preferred_element_type=F32) + jnp.dot(
        weight_low, back, preferred_element_type=F32
    )
    outv[...] = (mixed.astype(F32) + mixture).astype(BF16)
    store_out = pltpu.make_async_copy(outv, out_h, lsem.at[len(copies) + 1])
    store_out.start()

    settle(xin.at[pl.ds(0, (zc - 1) * seqs)], ssem.at[1])
    settle(pbuf.at[pl.ds(0, (zc - 1) * seqs)], ssem.at[2])
    settle(qbuf.at[pl.ds(0, (zc - 1) * seqs)], ssem.at[10])
    settle(oin.at[pl.ds(0, tc - 1)], ssem.at[4])
    settle(rin.at[pl.ds(0, (ec - 1) * cap)], ssem.at[5])
    settle(xg.at[pl.ds(0, ny - 1)], ssem.at[6])
    settle(xg.at[pl.ds(0, (nx - 1) * ny)], ssem.at[7])
    settle(hin.at[pl.ds(0, tc - 1)], ssem.at[8])
    settle(rin.at[pl.ds(0, (ec - 1) * cap)], ssem.at[9])
    store_state.wait()
    store_out.wait()


def hand_over(out_h, state_h, out_to, state_to, outv, state, sem):
    pieces = 8
    rows = state.shape[0] // pieces
    ins = [pltpu.make_async_copy(out_h, outv, sem.at[0])]
    outs = [pltpu.make_async_copy(outv, out_to, sem.at[1])]
    for i in range(pieces):
        part = pl.ds(i * rows, rows)
        ins.append(
            pltpu.make_async_copy(state_h.at[part], state.at[part], sem.at[2 + 2 * i])
        )
        outs.append(
            pltpu.make_async_copy(state.at[part], state_to.at[part], sem.at[3 + 2 * i])
        )
    for copy in ins:
        copy.start()
    for arriving, leaving in zip(ins, outs):
        arriving.wait()
        leaving.start()
    for copy in outs:
        copy.wait()


def on_device(ec, tc, nx, *args):
    (
        stream,
        previous_state,
        mixer_norm_gain,
        query_matrix,
        key_matrix,
        value_matrix,
        output_gate_weight,
        decay_lower_factor,
        decay_upper_factor,
        forgetting_boost,
        head_norm_gain,
        output_matrix,
        mixture_norm_gain,
        expert_gate_weight,
        expert_up_weight,
        expert_down_weight,
        expert_index_table,
        expert_scores_within,
        group_probability,
    ) = args
    seqs, width = stream.shape
    cap = 2 * seqs * expert_index_table.shape[1] // ec
    slots = ec * cap
    units = expert_gate_weight.shape[1]
    ff = expert_down_weight.shape[1]
    zc = ec // 2
    operands = (
        stream,
        previous_state,
        mixer_norm_gain.reshape(1, width),
        query_matrix,
        key_matrix,
        value_matrix,
        output_gate_weight,
        decay_lower_factor.T,
        decay_upper_factor,
        forgetting_boost,
        head_norm_gain.reshape(1, DV),
        output_matrix,
        mixture_norm_gain.reshape(1, width),
        expert_gate_weight,
        expert_up_weight,
        expert_down_weight,
        expert_index_table.T,
        expert_scores_within.T,
        group_probability.reshape(1, seqs),
    )
    v = pltpu.VMEM
    scratch = [
        v((seqs, width), BF16),
        v(previous_state.shape, F32),
        v((1, width), F32),
        v((W, 4 * W), BF16),
        v((2 * W, 3 * W), BF16),
        v(decay_lower_factor.shape[::-1], BF16),
        v((decay_upper_factor.shape[0], W), BF16),
        v((seqs, W), F32),
        v((1, DV), F32),
        v(output_matrix.shape, BF16),
        v((1, width), F32),
        v((2, units, width), BF16),
        v((ff, W), BF16),
        v(expert_index_table.shape[::-1], jnp.int32),
        v(expert_scores_within.shape[::-1], F32),
        v((1, seqs), F32),
        v((zc * seqs, 2 * W), BF16),
        v((zc * seqs, 2 * W), BF16),
        v((zc * seqs, 2 * W), BF16),
        v((zc * seqs, W), BF16),
        v((zc * seqs, W), BF16),
        v((2, seqs, W), F32),
        v((2, seqs, W), F32),
        v((seqs, width), BF16),
        v((tc, seqs, W), BF16),
        v((slots, W), BF16),
        v((slots, W), BF16),
        v((tc, slots, W), BF16),
        v((8 * units, width), BF16),
        v((4, ff, W), BF16),
        v((tc, slots // 4, W), BF16),
        v((slots, W), BF16),
        v((slots, W), BF16),
        v((seqs, W), F32),
        v((seqs, W), BF16),
        v((W, seqs), F32),
        v((seqs, slots), F32),
        v((slots, seqs), BF16),
        pltpu.SemaphoreType.DMA((21,)),
        pltpu.SemaphoreType.DMA((12,)),
        pltpu.SemaphoreType.DMA((10,)),
        pltpu.SemaphoreType.DMA((zc,)),
        pltpu.SemaphoreType.DMA((tc,)),
    ]
    hbm = pl.BlockSpec(memory_space=pltpu.HBM)
    results = pl.pallas_call(
        functools.partial(kernel, ec, tc, nx, cap),
        out_shape=(
            jax.ShapeDtypeStruct((seqs, W), BF16),
            jax.ShapeDtypeStruct(previous_state.shape, F32),
        ),
        in_specs=[hbm] * len(operands),
        out_specs=(hbm, hbm),
        scratch_shapes=scratch,
        compiler_params=pltpu.CompilerParams(
            collective_id=0, has_side_effects=True, vmem_limit_bytes=67043328
        ),
        name="layer",
    )(*operands)
    return pl.pallas_call(
        hand_over,
        out_shape=[jax.ShapeDtypeStruct(a.shape, a.dtype) for a in results],
        in_specs=[hbm] * 2,
        out_specs=[hbm] * 2,
        scratch_shapes=[
            v((seqs, W), BF16),
            v(previous_state.shape, F32),
            pltpu.SemaphoreType.DMA((18,)),
        ],
        compiler_params=pltpu.CompilerParams(vmem_limit_bytes=67043328),
        name="hand_over",
    )(*results)


def solution(mesh):
    ec, tc = mesh.shape["ep"], mesh.shape["tp"]
    placed = (
        P("ep", None),
        P("ep", None, "tp"),
        P(),
        P("ep", None),
        P("ep", None),
        P("ep", "tp"),
        P("ep", "tp"),
        P(),
        P(),
        P("ep", None),
        P(),
        P("tp", None),
        P(),
        P("ep", "tp", None),
        P("ep", "tp", None),
        P("ep", None, "tp"),
        P("ep", None),
        P("ep", None),
        P("ep"),
    )
    return jax.shard_map(
        functools.partial(on_device, ec, tc, min(NX, tc // 2)),
        mesh=mesh,
        in_specs=placed,
        out_specs=(P("ep", "tp"), P("ep", None, "tp")),
        check_vma=False,
    )
```

```python
import functools

import jax
import jax.numpy as jnp
from jax import lax
from jax.experimental import pallas as pl
from jax.experimental.pallas import tpu as pltpu
from jax.sharding import PartitionSpec as P

KEY_CHANNELS = 128
DV = 256
W = 128
NX = 4
EPSILON = 1e-06
SOFTNESS = 16.0
MESH = pl.DeviceIdType.MESH
F32 = jnp.float32
BF16 = jnp.bfloat16


def aligned(index, size):
    return pl.ds(pl.multiple_of(index * size, size), size)


def kernel(
    ec,
    tc,
    nx,
    cap,
    stream_h,
    state_h,
    gain1_h,
    query_h,
    key_h,
    value_h,
    gate_h,
    lower_h,
    upper_h,
    boost_h,
    hgain_h,
    wo_h,
    gain2_h,
    eg_h,
    eu_h,
    ed_h,
    ids_h,
    scores_h,
    prob_h,
    out_h,
    newstate_h,
    stream,
    state,
    gain1,
    wraw,
    wcat,
    lower,
    upper,
    boost,
    hgain,
    wo,
    gain2,
    egu,
    ed,
    ids,
    scores,
    prob,
    xin,
    pbuf,
    pin,
    qbuf,
    qin,
    qkb,
    ssb,
    obuf,
    oin,
    dbuf,
    rin,
    xg,
    w4,
    wdp,
    hin,
    rbuf,
    retin,
    ro,
    outv,
    factor_t,
    comb,
    disp,
    lsem,
    ssem,
    rsem,
    xsem,
    bsem,
):
    ep = lax.axis_index("ep")
    tp = lax.axis_index("tp")
    zc = ec // 2
    ny = tc // nx
    z = ep // 2
    core = ep % 2
    y = tp // nx
    x = tp % nx
    heads_before = tp * W // DV
    half = tp % (DV // W)
    seqs, width = stream.shape
    units = eg_h.shape[1]
    ff = units * tc
    slots = ec * cap

    barrier = pltpu.get_barrier_semaphore()

    def every_ep(put):
        def chip(to):
            put(to * 2 + 1 - core)
            put(to * 2 + core)

        def pair(i, carry):
            d = zc // 2 - i
            chip(lax.rem(z + d, zc))
            chip(lax.rem(z + zc - d, zc))
            return carry

        chip(lax.rem(z + zc // 2, zc))
        lax.fori_loop(1, zc // 2, pair, 0)
        put(ep + 1 - 2 * core)

    offsets = sorted(range(nx), key=lambda o: -min(o, nx - o))
    columns = [lax.rem(x + o, nx) for o in offsets]

    def every_tp(put):
        def row(to):
            for column in columns:
                put(to * nx + column)

        def pair(i, carry):
            d = ny // 2 - i
            row(lax.rem(y + d, ny))
            row(lax.rem(y + ny - d, ny))
            return carry

        row(lax.rem(y + ny // 2, ny))
        lax.fori_loop(1, ny // 2, pair, 0)
        for column in columns[:-1]:
            put(y * nx + column)

    def greet(device):
        pl.semaphore_signal(barrier, inc=1, device_id=device, device_id_type=MESH)

    every_ep(lambda to: greet((to, tp)))

    copies = {}

    def load(name, src, dst):
        cp = pltpu.make_async_copy(src, dst, lsem.at[len(copies)])
        cp.start()
        copies[name] = cp

    head_cols = aligned(heads_before, W)
    load("stream", stream_h, stream)
    load("gain1", gain1_h, gain1)
    load("wq", query_h.at[:, head_cols], wraw.at[:, pl.ds(0, W)])
    load("wk", key_h.at[:, head_cols], wraw.at[:, pl.ds(W, W)])
    load("wv", value_h, wraw.at[:, pl.ds(2 * W, W)])
    load("wg", gate_h, wraw.at[:, pl.ds(3 * W, W)])
    load("lower", lower_h, lower)
    load("upper", upper_h.at[:, head_cols], upper)
    load("boost", boost_h.at[:, head_cols], boost)
    load("state", state_h, state)
    load("ids", ids_h, ids)
    load("scores", scores_h, scores)
    load("prob", prob_h, prob)
    load("hgain", hgain_h, hgain)
    load("wo", wo_h, wo)
    load("gain2", gain2_h, gain2)
    load("eg", eg_h.at[0], egu.at[0])
    load("eu", eu_h.at[0], egu.at[1])
    load("ed", ed_h.at[0], ed)

    every_tp(lambda to: greet((ep, to)))

    def arrive(*names):
        for name in names:
            copies[name].wait()

    def settle(ref, sem):
        pltpu.make_async_copy(ref, ref, sem).wait()

    arrive("gain1", "wq", "wk", "wv", "wg")
    gain_row = gain1[:, aligned(ep, W)]
    gain_col = jnp.transpose(jnp.broadcast_to(gain_row, (W, W)))
    first_half = half == 0
    shared = jnp.where(
        first_half, wraw[:, :W].astype(F32), wraw[:, W : 2 * W].astype(F32)
    )
    wcat[aligned(core, W), :W] = (shared * gain_col).astype(BF16)
    gain_wide = jnp.concatenate([gain_col] * 2, axis=1)
    wcat[aligned(core, W), W:] = (wraw[:, 2 * W :].astype(F32) * gain_wide).astype(BF16)

    arrive("stream")
    rows = stream[...].astype(F32)
    scale1 = lax.rsqrt(jnp.mean(rows * rows, axis=1, keepdims=True) + EPSILON)
    normed = (rows * scale1 * gain1[...]).astype(BF16)

    pl.semaphore_wait(barrier, ec + tc - 2)

    def send(src, dst, sent, received, device):
        pltpu.make_async_remote_copy(
            src_ref=src,
            dst_ref=dst,
            send_sem=sent,
            recv_sem=received,
            device_id=device,
            device_id_type=MESH,
        ).start()

    half_rows = wcat.at[aligned(core, W)]
    send(half_rows, half_rows, ssem.at[0], rsem.at[0], (ep + 1 - 2 * core, tp))
    chip_width = 2 * W

    def send_x(to):
        send(
            stream.at[:, aligned(to, chip_width)],
            xin.at[aligned(z, seqs)],
            ssem.at[1],
            xsem.at[z],
            (to * 2 + core, tp),
        )

    send_x((z + zc // 2) % zc)

    def send_x_pair(i, carry):
        d = zc // 2 - i
        send_x((z + d) % zc)
        send_x((z + zc - d) % zc)
        return carry

    lax.fori_loop(1, zc // 2, send_x_pair, 0)

    arrive("lower", "upper", "boost")
    low = lax.dot_general(
        normed, lower[...], (((1,), (1,)), ((), ())), preferred_element_type=F32
    ).astype(BF16)
    logit = jnp.dot(low, upper[...], preferred_element_type=F32)
    lograte = jax.nn.log_sigmoid(logit) / SOFTNESS - boost[...]
    factor_t[...] = jnp.transpose(jnp.exp(lograte))

    arrive("ids", "scores", "prob")
    lane = lax.broadcasted_iota(jnp.int32, (seqs, slots), 1)
    mine = (lane // cap).astype(F32)
    diagonal = lax.broadcasted_iota(jnp.int32, (seqs, seqs), 0) == lax.broadcasted_iota(
        jnp.int32, (seqs, seqs), 1
    )

    def column(row):
        square = jnp.where(diagonal, jnp.broadcast_to(row, (seqs, seqs)), 0.0)
        return jnp.sum(square, axis=1, keepdims=True)

    first = jnp.where(column(ids[0:1, :].astype(F32)) == mine, 1.0, 0.0)
    second = jnp.where(column(ids[1:2, :].astype(F32)) == mine, 1.0, 0.0)
    either = first + second
    before = jnp.where(
        lax.broadcasted_iota(jnp.int32, (seqs, seqs), 1)
        < lax.broadcasted_iota(jnp.int32, (seqs, seqs), 0),
        1.0,
        0.0,
    )
    earlier = jnp.dot(
        before.astype(BF16), either.astype(BF16), preferred_element_type=F32
    )
    chosen = jnp.where(jnp.abs(earlier - (lane % cap).astype(F32)) < 0.5, either, 0.0)
    disp[...] = jnp.transpose(chosen).astype(BF16)
    raised = jnp.exp(scores[...])
    weights = raised / jnp.sum(raised, axis=0, keepdims=True) * prob[...]
    comb[...] = chosen * (first * column(weights[0:1, :]) + second * column(weights[1:2, :]))

    pltpu.make_async_remote_copy(
        src_ref=half_rows,
        dst_ref=wcat.at[aligned(1 - core, W)],
        send_sem=ssem.at[0],
        recv_sem=rsem.at[0],
        device_id=(ep + 1 - 2 * core, tp),
        device_id_type=MESH,
    ).wait()

    xin[aligned(z, seqs), :] = stream[:, aligned(z, chip_width)]

    qin[aligned(z, seqs), :] = jnp.dot(
        xin[aligned(z, seqs), :], wcat[:, :W], preferred_element_type=F32
    ).astype(BF16)

    def send_q(to):
        send(
            qbuf.at[aligned(to, seqs)],
            qin.at[aligned(z, seqs)],
            ssem.at[10],
            rsem.at[8],
            (to * 2 + core, tp),
        )

    def answer_pair(d, carry):
        above = (z + d) % zc
        below = (z + zc - d) % zc
        settle(xin.at[aligned(above, seqs)], xsem.at[above])
        settle(xin.at[aligned(below, seqs)], xsem.at[below])
        pair = jnp.concatenate(
            [xin[aligned(above, seqs), :], xin[aligned(below, seqs), :]], axis=0
        )
        sums = jnp.dot(pair, wcat[:, :W], preferred_element_type=F32).astype(BF16)
        qbuf[aligned(above, seqs), :] = sums[:seqs]
        qbuf[aligned(below, seqs), :] = sums[seqs:]
        send_q(above)
        send_q(below)
        return carry

    lax.fori_loop(1, zc // 2, answer_pair, 0)
    across = (z + zc // 2) % zc
    settle(xin.at[aligned(across, seqs)], xsem.at[across])
    qbuf[aligned(across, seqs), :] = jnp.dot(
        xin[aligned(across, seqs), :], wcat[:, :W], preferred_element_type=F32
    ).astype(BF16)
    send_q(across)

    pbuf[...] = jnp.dot(xin[...], wcat[:, W:], preferred_element_type=F32).astype(BF16)

    def send_p(to):
        send(
            pbuf.at[aligned(to, seqs)],
            pin.at[aligned(z, seqs)],
            ssem.at[2],
            rsem.at[1],
            (to * 2 + core, tp),
        )

    send_p(across)

    def send_p_pair(i, carry):
        d = zc // 2 - i
        send_p((z + d) % zc)
        send_p((z + zc - d) % zc)
        return carry

    lax.fori_loop(1, zc // 2, send_p_pair, 0)
    pin[aligned(z, seqs), :] = pbuf[aligned(z, seqs), :]

    arrive("state")
    for s in range(seqs):
        state[s] = state[s] * factor_t[:, s : s + 1]

    arrive("gain2", "eg", "eu")
    for which in range(2):
        scaled = (egu[which].astype(F32) * gain2[...]).astype(BF16)
        for copy in range(4):
            w4[pl.ds((which * 4 + copy) * units, units), :] = scaled
    arrive("ed")
    for g in range(4):
        for block in range(ff // units):
            source = block // 4 * 4 + (block % 4 - g) % 4
            wdp[g, pl.ds(block * units, units), :] = ed[pl.ds(source * units, units), :]
    arrive("hgain", "wo")

    settle(qin.at[pl.ds(0, (zc - 1) * seqs)], rsem.at[8])
    own_sum = qin[pl.ds(0, seqs), :].astype(F32)
    for i in range(1, zc):
        own_sum = own_sum + qin[pl.ds(i * seqs, seqs), :].astype(F32)
    partner = tp + 1 - 2 * half
    qkb[0] = own_sum * scale1
    swap = pltpu.make_async_remote_copy(
        src_ref=qkb.at[0],
        dst_ref=qkb.at[1],
        send_sem=ssem.at[11],
        recv_sem=rsem.at[9],
        device_id=(ep, partner),
        device_id_type=MESH,
    )
    swap.start()

    settle(pin.at[pl.ds(0, (zc - 1) * seqs)], rsem.at[1])
    total = pin[pl.ds(0, seqs), :].astype(F32)
    for i in range(1, zc):
        total = total + pin[pl.ds(i * seqs, seqs), :].astype(F32)
    total = total * scale1
    swap.wait()

    query_rows = jnp.where(first_half, qkb[0], qkb[1])
    key_rows = jnp.where(first_half, qkb[1], qkb[0])
    query_t = jnp.transpose(query_rows * KEY_CHANNELS**-0.5)
    key_t = jnp.transpose(key_rows)
    value_rows = total[:, :W]
    gate_rows = total[:, W:]
    for s in range(seqs):
        fresh = state[s] + key_t[:, s : s + 1] * value_rows[s : s + 1, :]
        state[s] = fresh
        ro[s : s + 1, :] = jnp.sum(query_t[:, s : s + 1] * fresh, axis=0, keepdims=True)
    readout = ro[...]
    squares = jnp.sum(readout * readout, axis=1, keepdims=True)
    ssb[0] = jnp.broadcast_to(squares, (seqs, W))
    gated = (
        readout * hgain[:, aligned(half, W)] * (gate_rows * jax.nn.sigmoid(gate_rows))
    ).astype(BF16)
    exchange = pltpu.make_async_remote_copy(
        src_ref=ssb.at[0],
        dst_ref=ssb.at[1],
        send_sem=ssem.at[3],
        recv_sem=rsem.at[2],
        device_id=(ep, partner),
        device_id_type=MESH,
    )
    exchange.start()
    partial = jnp.dot(gated, wo[...], preferred_element_type=F32)
    store_state = pltpu.make_async_copy(state, newstate_h, lsem.at[len(copies)])
    store_state.start()
    exchange.wait()
    head_scale = lax.rsqrt((squares + ssb[1, :, 0:1]) / DV + EPSILON)
    obuf[...] = (partial * head_scale).astype(BF16)

    def send_o(to):
        send(obuf.at[:, aligned(to, W)], oin.at[tp], ssem.at[4], rsem.at[3], (ep, to))

    every_tp(send_o)
    oin[tp] = obuf[:, aligned(tp, W)]
    settle(oin.at[pl.ds(0, tc - 1)], rsem.at[3])
    mixed = stream[:, aligned(tp, W)].astype(F32)
    summed = oin[0].astype(F32)
    for i in range(1, tc):
        summed = summed + oin[i].astype(F32)
    mixed = (mixed + summed).astype(BF16)

    dbuf[...] = jnp.dot(disp[...], mixed, preferred_element_type=F32).astype(BF16)

    def send_d(to):
        send(
            dbuf.at[aligned(to, cap)],
            rin.at[aligned(ep, cap)],
            ssem.at[5],
            rsem.at[4],
            (to, tp),
        )

    every_ep(send_d)
    own = lax.broadcasted_iota(jnp.int32, (slots, W), 0) // cap == ep
    settle(rin.at[pl.ds(0, (ec - 1) * cap)], rsem.at[4])
    xg[tp] = jnp.where(own, dbuf[...].astype(F32), rin[...].astype(F32)).astype(BF16)

    def from_row(i):
        return (y + ny + (2 * (i % 2) - 1) * ((i + 1) // 2)) % ny

    def send_y(i, carry):
        to = from_row(i) * nx + x
        send(xg.at[tp], xg.at[tp], ssem.at[6], bsem.at[tp], (ep, to))
        return carry

    lax.fori_loop(1, ny, send_y, 0)

    def pass_x(block):
        for i in range(1, nx):
            to = y * nx + (x + i) % nx
            send(xg.at[block], xg.at[block], ssem.at[7], bsem.at[block], (ep, to))

    pass_x(tp)

    def forward(i, carry):
        block = from_row(i) * nx + x
        settle(xg.at[block], bsem.at[block])
        pass_x(block)
        return carry

    lax.fori_loop(1, ny, forward, 0)

    def products(i, carry):
        both, square = carry
        row = from_row(i) * nx
        for k in range(1, nx):
            block = row + (x + k) % nx
            settle(xg.at[block], bsem.at[block])
        pieces = [xg[row + k] for k in range(nx)]
        for piece in pieces:
            floats = piece.astype(F32)
            square = square + floats * floats
        both = both + lax.dot_general(
            jnp.concatenate(pieces, axis=1),
            w4[:, aligned(from_row(i), nx * W)],
            (((1,), (1,)), ((), ())),
            preferred_element_type=F32,
        )
        return both, square

    both, square = lax.fori_loop(
        0,
        ny,
        products,
        (jnp.zeros((slots, 8 * units), F32), jnp.zeros((slots, W), F32)),
    )
    scale2 = lax.rsqrt(jnp.sum(square, axis=1, keepdims=True) / width + EPSILON)
    gate_pre = both[:, : 4 * units] * scale2
    up_pre = both[:, 4 * units :] * scale2
    hidden = gate_pre * jax.nn.sigmoid(gate_pre) * up_pre
    group = slots // 4
    quarter = lax.broadcasted_iota(jnp.int32, (group, W), 1) // units
    tile = jnp.zeros((group, W), F32)
    for g in range(4):
        tile = jnp.where(
            quarter == (g + tp % 4) % 4, hidden[g * group : (g + 1) * group, :], tile
        )
    hin[tp] = tile.astype(BF16)

    def send_h(to):
        send(hin.at[tp], hin.at[tp], ssem.at[8], rsem.at[6], (ep, to))

    every_tp(send_h)
    settle(hin.at[pl.ds(0, tc - 1)], rsem.at[6])

    for g in range(4):
        pieces = []
        for a in range(tc // 4):
            piece = hin[4 * a].astype(F32)
            for b in range(1, 4):
                piece = jnp.where(
                    quarter == (g + b) % 4, hin[4 * a + b].astype(F32), piece
                )
            pieces.append(piece.astype(BF16))
        rbuf[pl.ds(g * group, group), :] = jnp.dot(
            jnp.concatenate(pieces, axis=1), wdp[g], preferred_element_type=F32
        ).astype(BF16)

    def send_r(to):
        send(
            rbuf.at[aligned(to, cap)],
            retin.at[aligned(ep, cap)],
            ssem.at[9],
            rsem.at[7],
            (to, tp),
        )

    every_ep(send_r)
    weight_high = comb[...].astype(BF16)
    weight_low = (comb[...] - weight_high.astype(F32)).astype(BF16)
    settle(retin.at[pl.ds(0, (ec - 1) * cap)], rsem.at[7])
    back = jnp.where(own, rbuf[...].astype(F32), retin[...].astype(F32)).astype(BF16)
    mixture = jnp.dot(weight_high, back, preferred_element_type=F32) + jnp.dot(
        weight_low, back, preferred_element_type=F32
    )
    outv[...] = (mixed.astype(F32) + mixture).astype(BF16)
    store_out = pltpu.make_async_copy(outv, out_h, lsem.at[len(copies) + 1])
    store_out.start()

    settle(xin.at[pl.ds(0, (zc - 1) * seqs)], ssem.at[1])
    settle(pbuf.at[pl.ds(0, (zc - 1) * seqs)], ssem.at[2])
    settle(qbuf.at[pl.ds(0, (zc - 1) * seqs)], ssem.at[10])
    settle(oin.at[pl.ds(0, tc - 1)], ssem.at[4])
    settle(rin.at[pl.ds(0, (ec - 1) * cap)], ssem.at[5])
    settle(xg.at[pl.ds(0, ny - 1)], ssem.at[6])
    settle(xg.at[pl.ds(0, (nx - 1) * ny)], ssem.at[7])
    settle(hin.at[pl.ds(0, tc - 1)], ssem.at[8])
    settle(rin.at[pl.ds(0, (ec - 1) * cap)], ssem.at[9])
    store_state.wait()
    store_out.wait()


def hand_over(out_h, state_h, out_to, state_to, outv, state, sem):
    pieces = 8
    rows = state.shape[0] // pieces
    ins = [pltpu.make_async_copy(out_h, outv, sem.at[0])]
    outs = [pltpu.make_async_copy(outv, out_to, sem.at[1])]
    for i in range(pieces):
        part = pl.ds(i * rows, rows)
        ins.append(
            pltpu.make_async_copy(state_h.at[part], state.at[part], sem.at[2 + 2 * i])
        )
        outs.append(
            pltpu.make_async_copy(state.at[part], state_to.at[part], sem.at[3 + 2 * i])
        )
    for copy in ins:
        copy.start()
    for arriving, leaving in zip(ins, outs):
        arriving.wait()
        leaving.start()
    for copy in outs:
        copy.wait()


def on_device(ec, tc, nx, *args):
    (
        stream,
        previous_state,
        mixer_norm_gain,
        query_matrix,
        key_matrix,
        value_matrix,
        output_gate_weight,
        decay_lower_factor,
        decay_upper_factor,
        forgetting_boost,
        head_norm_gain,
        output_matrix,
        mixture_norm_gain,
        expert_gate_weight,
        expert_up_weight,
        expert_down_weight,
        expert_index_table,
        expert_scores_within,
        group_probability,
    ) = args
    seqs, width = stream.shape
    cap = 2 * seqs * expert_index_table.shape[1] // ec
    slots = ec * cap
    units = expert_gate_weight.shape[1]
    ff = expert_down_weight.shape[1]
    zc = ec // 2
    operands = (
        stream,
        previous_state,
        mixer_norm_gain.reshape(1, width),
        query_matrix,
        key_matrix,
        value_matrix,
        output_gate_weight,
        decay_lower_factor.T,
        decay_upper_factor,
        forgetting_boost,
        head_norm_gain.reshape(1, DV),
        output_matrix,
        mixture_norm_gain.reshape(1, width),
        expert_gate_weight,
        expert_up_weight,
        expert_down_weight,
        expert_index_table.T,
        expert_scores_within.T,
        group_probability.reshape(1, seqs),
    )
    v = pltpu.VMEM
    scratch = [
        v((seqs, width), BF16),
        v(previous_state.shape, F32),
        v((1, width), F32),
        v((W, 4 * W), BF16),
        v((2 * W, 3 * W), BF16),
        v(decay_lower_factor.shape[::-1], BF16),
        v((decay_upper_factor.shape[0], W), BF16),
        v((seqs, W), F32),
        v((1, DV), F32),
        v(output_matrix.shape, BF16),
        v((1, width), F32),
        v((2, units, width), BF16),
        v((ff, W), BF16),
        v(expert_index_table.shape[::-1], jnp.int32),
        v(expert_scores_within.shape[::-1], F32),
        v((1, seqs), F32),
        v((zc * seqs, 2 * W), BF16),
        v((zc * seqs, 2 * W), BF16),
        v((zc * seqs, 2 * W), BF16),
        v((zc * seqs, W), BF16),
        v((zc * seqs, W), BF16),
        v((2, seqs, W), F32),
        v((2, seqs, W), F32),
        v((seqs, width), BF16),
        v((tc, seqs, W), BF16),
        v((slots, W), BF16),
        v((slots, W), BF16),
        v((tc, slots, W), BF16),
        v((8 * units, width), BF16),
        v((4, ff, W), BF16),
        v((tc, slots // 4, W), BF16),
        v((slots, W), BF16),
        v((slots, W), BF16),
        v((seqs, W), F32),
        v((seqs, W), BF16),
        v((W, seqs), F32),
        v((seqs, slots), F32),
        v((slots, seqs), BF16),
        pltpu.SemaphoreType.DMA((21,)),
        pltpu.SemaphoreType.DMA((12,)),
        pltpu.SemaphoreType.DMA((10,)),
        pltpu.SemaphoreType.DMA((zc,)),
        pltpu.SemaphoreType.DMA((tc,)),
    ]
    hbm = pl.BlockSpec(memory_space=pltpu.HBM)
    results = pl.pallas_call(
        functools.partial(kernel, ec, tc, nx, cap),
        out_shape=(
            jax.ShapeDtypeStruct((seqs, W), BF16),
            jax.ShapeDtypeStruct(previous_state.shape, F32),
        ),
        in_specs=[hbm] * len(operands),
        out_specs=(hbm, hbm),
        scratch_shapes=scratch,
        compiler_params=pltpu.CompilerParams(
            collective_id=0, has_side_effects=True, vmem_limit_bytes=67043328
        ),
        name="layer",
    )(*operands)
    return pl.pallas_call(
        hand_over,
        out_shape=[jax.ShapeDtypeStruct(a.shape, a.dtype) for a in results],
        in_specs=[hbm] * 2,
        out_specs=[hbm] * 2,
        scratch_shapes=[
            v((seqs, W), BF16),
            v(previous_state.shape, F32),
            pltpu.SemaphoreType.DMA((18,)),
        ],
        compiler_params=pltpu.CompilerParams(vmem_limit_bytes=67043328),
        name="hand_over",
    )(*results)


def solution(mesh):
    ec, tc = mesh.shape["ep"], mesh.shape["tp"]
    placed = (
        P("ep", None),
        P("ep", None, "tp"),
        P(),
        P("ep", None),
        P("ep", None),
        P("ep", "tp"),
        P("ep", "tp"),
        P(),
        P(),
        P("ep", None),
        P(),
        P("tp", None),
        P(),
        P("ep", "tp", None),
        P("ep", "tp", None),
        P("ep", None, "tp"),
        P("ep", None),
        P("ep", None),
        P("ep"),
    )
    return jax.shard_map(
        functools.partial(on_device, ec, tc, min(NX, tc // 2)),
        mesh=mesh,
        in_specs=placed,
        out_specs=(P("ep", "tp"), P("ep", None, "tp")),
        check_vma=False,
    )
```
